32 devices in a mesh: kv: 8 (over z, y), tp: 4 (over x, core).
Axes of the slice: x: 2, y: 2, z: 4, core: 2. Of those that a mesh axis runs over, the one named last changes fastest.
Arguments:
- tokens: bfloat16 [128, 4, 4096], P(None, None, ('kv', 'tp')), may hold values from -6 to 6
- input_norm_gain: float32 [4096], replicated, may hold values from 0.1 to 1.9
- w_query: bfloat16 [4096, 4096], P(None, 'kv'), may hold values from -0.09375 to 0.09375
- w_forget: bfloat16 [4096, 4096], P(None, 'kv'), may hold values from -0.09375 to 0.09375
- w_input: bfloat16 [32, 128, 4096], P('kv', 'tp'), may hold values from -0.09375 to 0.09375
- w_gate: bfloat16 [32, 128, 4096], P('kv', 'tp'), may hold values from -0.09375 to 0.09375
- forget_floor: float32 [4096], P('kv'), may hold values from 0 to 0.95
- head_gain: float32 [128], P('tp'), may hold values from 0.1 to 1.9
- w_out: bfloat16 [4096, 4096], P('kv'), may hold values from -0.09375 to 0.09375
- state: float32 [128, 32, 128, 128], P(None, 'kv', 'tp'), may hold values from -12 to 12
- prev_forget: float32 [128, 4, 4096], P(None, None, 'kv'), may hold values from 0.2 to 1
- prev_input: bfloat16 [128, 4, 32, 128], P(None, None, 'kv', 'tp'), may hold values from -6 to 6
- accepted: int32 [128], replicated, may hold values from 0 to 4
Outputs:
- mixed: bfloat16 [128, 4, 4096], P(None, None, ('kv', 'tp'))
- new_state: float32 [128, 32, 128, 128], P(None, 'kv', 'tp')
The draws below stay inside these ranges and needn't reach their ends.
All inputs are finite; a program needn't handle non-finite values.
Results may differ from the reference program's by a relative error of at most 0.019.
Values may be sent and summed in bfloat16 or wider, within the bound.
A program may use at most 128 MiB of HBM per device.

```python
import jax
import jax.numpy as jnp
from jax import lax

D = 4096
HD = 128
HEADS = 32
PROP = 4
SEQS = 128


def draw_state(key, part):
    heads = D // HD
    shape = (SEQS, heads, HD, HD)
    rising = (0.5 * 3.0 ** (jnp.arange(HD, dtype=jnp.float32) / (HD - 1))).reshape(HD, 1)
    base = jnp.clip(jax.random.normal(jax.random.fold_in(key, 13), shape, jnp.float32), -4.0, 4.0)
    values = base * rising
    return jnp.clip(values, -12.0, 12.0).astype(jnp.float32)


def set_ends(values, rng, least, largest):
    place = [jax.random.randint(jax.random.fold_in(rng, axis), (), 0, length) for axis, length in enumerate(values.shape)]
    main_axis = values.shape.index(max(values.shape))
    neighbour = place[:main_axis] + [(place[main_axis] + 1) % values.shape[main_axis]] + place[main_axis + 1:]
    return values.at[tuple(place)].set(least).at[tuple(neighbour)].set(largest)


def level_of(own_key, extent, shards, least, high):
    def one(dim, parts):
        heights = jax.random.uniform(jax.random.fold_in(jax.random.fold_in(own_key, 6), dim), (parts,), jnp.float32, least / len(shards), high / len(shards))
        return jnp.repeat(jnp.exp(heights), extent[dim] // parts).reshape((-1,) + (1,) * (len(extent) - dim - 1))

    level = one(*shards[0])
    for cut in shards[1:]:
        level = level * one(*cut)
    return level


def gaussian(key, shape, width, bound, pieces=(), held_as=jnp.bfloat16):
    values = width * jax.random.normal(key, shape, jnp.float32)
    if pieces:
        values = values * level_of(key, shape, pieces, -0.22, 0.18)
    return jnp.clip(values, -bound, bound).astype(held_as)


def setup_inputs(seed: int = 0) -> dict:
    key_list = jax.random.split(jax.random.key(seed), 14)
    return {
        "tokens": gaussian(key_list[0], (SEQS, PROP, D), 1.0, 6.0, ((2, 32),)),
        "input_norm_gain": jnp.clip(1.0 + 0.18 * jax.random.normal(key_list[1], (D,), jnp.float32), 0.1, 1.9),
        "w_query": gaussian(key_list[2], (D, D), D ** -0.5, 0.09375, ((1, 8),)),
        "w_forget": gaussian(key_list[3], (D, D), D ** -0.5, 0.09375, ((1, 8),)),
        "w_input": gaussian(key_list[4], (HEADS, HD, D), D ** -0.5, 0.09375, ((0, 8), (1, 4))),
        "w_gate": gaussian(key_list[5], (HEADS, HD, D), D ** -0.5, 0.09375, ((0, 8), (1, 4))),
        "forget_floor": jnp.clip(0.95 * jax.random.uniform(key_list[6], (D,), jnp.float32) ** level_of(key_list[6], (D,), ((0, 8),), -0.2, 0.2), 0.0, 0.95),
        "head_gain": jnp.clip(1.0 + 0.18 * jax.random.normal(key_list[7], (HD,), jnp.float32), 0.1, 1.9),
        "w_out": gaussian(key_list[8], (D, D), D ** -0.5, 0.09375, ((0, 8),)),
        "state": draw_state(jax.random.fold_in(key_list[13], 71), 0),
        "prev_forget": jnp.clip(0.2 + 0.8 * jax.random.uniform(key_list[10], (SEQS, PROP, D), jnp.float32) ** level_of(key_list[10], (SEQS, PROP, D), ((2, 8),), -0.2, 0.2), 0.2, 1.0),
        "prev_input": gaussian(key_list[11], (SEQS, PROP, HEADS, HD), 1.0, 6.0, ((2, 8), (3, 4))),
        "accepted": set_ends(jax.random.randint(key_list[12], (SEQS,), 0, PROP + 1), jax.random.fold_in(key_list[12], 1), 0, PROP).astype(jnp.int32),
    }


NORM_EPSILON = 1e-06

def rms_scale(values, gain):
    return values * lax.rsqrt(lax.optimization_barrier(jnp.mean(values * values, axis=-1, keepdims=True)) + NORM_EPSILON) * gain

def reference(tokens, input_norm_gain, w_query, w_forget, w_input, w_gate, forget_floor, head_gain, w_out, state, prev_forget, prev_input, accepted):
    seq_count = tokens.shape[0]
    heads = D // HD
    row_count = seq_count * PROP
    normed = rms_scale(tokens.astype(jnp.float32), input_norm_gain).astype(jnp.bfloat16).reshape(row_count, D)

    def project(weight):
        return jnp.dot(normed, weight, preferred_element_type=jnp.float32).astype(jnp.bfloat16)
    queries = project(w_query)
    forget_raw = project(w_forget)
    input_proj = project(w_input.reshape(D, D).T)
    gate_raw = project(w_gate.reshape(D, D).T)
    forget = forget_floor + (1.0 - forget_floor) * jax.nn.sigmoid(forget_raw.astype(jnp.float32))

    def head_first(values):
        return values.astype(jnp.float32).reshape(seq_count, PROP, heads, HD).transpose(2, 0, 1, 3)

    def advance_head(inputs_all):
        start_state, prev_gate, earlier_values, query_vector, gate_now_all, fresh = inputs_all
        present_step = start_state
        for token_position in range(PROP):
            alive_mask = (token_position < accepted)[:, None, None]
            gate_now = prev_gate[:, token_position]
            update = gate_now[:, :, None] * present_step + (1.0 - gate_now)[:, :, None] * earlier_values[:, token_position][:, None, :]
            present_step = jnp.where(alive_mask, update, present_step)
        base_state = present_step
        output_tokens = []
        for token_position in range(PROP):
            gate_now = gate_now_all[:, token_position]
            present_step = gate_now[:, :, None] * present_step + (1.0 - gate_now)[:, :, None] * fresh[:, token_position][:, None, :]
            output_tokens.append(jnp.einsum('ue,uef->uf', query_vector[:, token_position], present_step))
        return (base_state, jnp.stack(output_tokens, axis=1))
    inputs_all = (state.transpose(1, 0, 3, 2), head_first(prev_forget), head_first(prev_input), head_first(queries), head_first(forget), head_first(input_proj))
    base_states, head_outputs = lax.map(advance_head, inputs_all)
    new_state = base_states.transpose(1, 0, 3, 2)
    heads_out = head_outputs.transpose(1, 2, 0, 3)
    gate_heads = gate_raw.astype(jnp.float32).reshape(seq_count, PROP, heads, HD)
    hidden = (rms_scale(heads_out, head_gain) * jax.nn.silu(gate_heads)).astype(jnp.bfloat16).reshape(row_count, D)
    mixed = jnp.dot(hidden, w_out, preferred_element_type=jnp.float32).astype(jnp.bfloat16).reshape(seq_count, PROP, D)
    return (mixed, new_state)
```

```python
import functools

import jax
import jax.numpy as jnp
from jax import lax
from jax.experimental import pallas as pl
from jax.experimental.pallas import tpu as pltpu
from jax.sharding import PartitionSpec as P

NORM_EPSILON = 1e-06
MESH = pl.DeviceIdType.MESH
VMEM_BYTES = 60 * 1024 * 1024
F32 = jnp.float32
BF16 = jnp.bfloat16


def contract(a, b, da, db):
    return lax.dot_general(a, b, (((da,), (db,)), ((), ())), preferred_element_type=F32)


def state_kernel(acc_ref, pf_ref, pv_ref, spread_ref, state_ref, new_ref, low_ref):
    prop, group, chans = pf_ref.shape
    heads, vals, keys = state_ref.shape[1:]
    wide = 8 * vals
    accepted = acc_ref[...]
    decay = jnp.ones((group, chans), F32)
    weights = [None] * prop
    for p in range(prop - 1, -1, -1):
        alive = p < accepted
        gate = pf_ref[p]
        weights[p] = jnp.where(alive, decay * (1.0 - gate), 0.0)
        decay = jnp.where(alive, decay * gate, decay)
    spread = [
        jnp.dot(pv_ref[p], spread_ref[...], preferred_element_type=F32) for p in range(prop)
    ]
    rows = lax.broadcasted_iota(jnp.int32, (8 * prop, wide), 0) % 8
    lanes = lax.broadcasted_iota(jnp.int32, (8 * prop, wide), 1) // vals
    mask = rows == lanes
    for g in range(group // 8):
        sl = slice(g * 8, g * 8 + 8)
        for h in range(heads):
            hk = slice(h * keys, (h + 1) * keys)
            lhs = jnp.concatenate(
                [spread[p][sl, h * wide : (h + 1) * wide] for p in range(prop)], axis=0
            )
            lhs = jnp.where(mask, lhs, 0.0).astype(BF16)
            rhs = jnp.concatenate([weights[p][sl, hk] for p in range(prop)], axis=0).astype(BF16)
            update = contract(lhs, rhs, 0, 0).reshape(8, vals, keys)
            new = decay[sl, hk][:, None, :] * state_ref[sl, h] + update
            new_ref[sl, h] = new
            low_ref[sl, h] = new.astype(BF16)


def update_state(accepted, prev_forget, prev_input, state):
    seqs, heads, vals, keys = state.shape
    prop = prev_forget.shape[1]
    group = 16
    pf = prev_forget.transpose(1, 0, 2)
    pv = prev_input.reshape(seqs, prop, heads * vals).transpose(1, 0, 2)
    r = jnp.arange(heads * vals)[:, None]
    c = jnp.arange(heads * 8 * vals)[None, :]
    spread = ((r // vals == c // (8 * vals)) & (r % vals == c % vals)).astype(BF16)
    block = (group, heads, vals, keys)
    return pl.pallas_call(
        state_kernel,
        grid=(seqs // group,),
        in_specs=[
            pl.BlockSpec((group, 1), lambda i: (i, 0)),
            pl.BlockSpec((prop, group, heads * keys), lambda i: (0, i, 0)),
            pl.BlockSpec((prop, group, heads * vals), lambda i: (0, i, 0)),
            pl.BlockSpec(spread.shape, lambda i: (0, 0)),
            pl.BlockSpec(block, lambda i: (i, 0, 0, 0)),
        ],
        out_specs=[
            pl.BlockSpec(block, lambda i: (i, 0, 0, 0)),
            pl.BlockSpec(block, lambda i: (i, 0, 0, 0)),
        ],
        out_shape=[
            jax.ShapeDtypeStruct(state.shape, F32),
            jax.ShapeDtypeStruct(state.shape, BF16),
        ],
        compiler_params=pltpu.CompilerParams(vmem_limit_bytes=VMEM_BYTES // 2),
        cost_estimate=pl.CostEstimate(
            flops=2 * 8 * prop * state.size, bytes_accessed=10 * state.size, transcendentals=0
        ),
    )(accepted.reshape(seqs, 1), pf, pv, spread, state)


def layer_kernel(
    kv_size,
    tp_size,
    tok_ref,
    gain_ref,
    floor_ref,
    hgain_ref,
    fold_ref,
    wq_hbm,
    wf_hbm,
    wi_hbm,
    wg_hbm,
    wo_hbm,
    st_hbm,
    out_ref,
    gath,
    wq,
    wf,
    wig,
    wo,
    st,
    acc,
    ss,
    qd,
    ho,
    pre,
    sq,
    rx,
    rsq,
    term,
    rt,
    w_sem,
    wo_sem,
    own_sem,
    z_send,
    a_send,
    b_send,
    d_send,
    slot_recv,
    d_recv,
    x_send,
    x_recv,
    s_send,
    s_recv,
    t_send,
    t_recv,
):
    n = kv_size * tp_size
    chips = n // 2
    zs = kv_size // 2
    kv = lax.axis_index("kv")
    tp = lax.axis_index("tp")
    me = kv * tp_size + tp
    z, y, x, c = kv // 2, kv % 2, tp // 2, tp % 2
    width = tok_ref.shape[1]
    rows = tok_ref.shape[0]
    seqs, heads, vals, keys = st_hbm.shape
    prop = rows // seqs
    hk = heads * keys
    hv = heads * vals
    features = n * width

    weight_copies = [
        pltpu.make_async_copy(wq_hbm, wq, w_sem.at[0]),
        pltpu.make_async_copy(wf_hbm, wf, w_sem.at[1]),
        pltpu.make_async_copy(wi_hbm, wig.at[pl.ds(0, hv)], w_sem.at[2]),
        pltpu.make_async_copy(wg_hbm, wig.at[pl.ds(hv, hv)], w_sem.at[3]),
    ]
    state_copy = pltpu.make_async_copy(st_hbm, st, w_sem.at[4])
    out_copies = [
        pltpu.make_async_copy(
            wo_hbm.at[pl.ds(h * keys + j * vals, vals)],
            wo.at[pl.ds((j * heads + h) * vals, vals)],
            wo_sem.at[h * tp_size + j],
        )
        for h in range(heads)
        for j in range(tp_size)
    ]

    def columns(zr, fy, fx, core):
        oz = (z + zr) % zs
        oy = y + fy * (1 - 2 * y)
        ox = x + fx * (1 - 2 * x)
        index = (oz * 2 + oy) * tp_size + ox * 2 + core
        return pl.ds(pl.multiple_of(index * width, width), width)

    own = pltpu.make_async_copy(tok_ref, gath.at[:, columns(0, 0, 0, c)], own_sem)
    own.start()

    barrier = pltpu.get_barrier_semaphore()

    @pl.loop(1, n)
    def _(d):
        other = (me + d) % n
        pl.semaphore_signal(
            barrier,
            inc=1,
            device_id=(other // tp_size, other % tp_size),
            device_id_type=MESH,
        )

    own.wait()
    pl.semaphore_wait(barrier, n - 1)

    def remote(view, send, recv, target):
        return pltpu.make_async_remote_copy(
            src_ref=view,
            dst_ref=view,
            send_sem=send,
            recv_sem=recv,
            device_id=target,
            device_id_type=MESH,
        )

    a_peer = (kv + (1 - c) * (1 - 2 * y), tp + c * (1 - 2 * x) * 2)
    b_peer = (kv + c * (1 - 2 * y), tp + (1 - c) * (1 - 2 * x) * 2)
    partner = (kv, tp + 1 - 2 * c)

    def flips(ar, br):
        return ar * (1 - c) + br * c, ar * c + br * (1 - c)

    def view(zr, ar, br):
        fy, fx = flips(ar, br)
        return gath.at[:, columns(zr, fy, fx, c)]

    def slot(zr, ar, br):
        fy, fx = flips(ar, br)
        return zr * 4 + fy * 2 + fx

    def to_z(zr):
        return remote(
            view(0, 0, 0),
            z_send.at[zr],
            slot_recv.at[zr * 4],
            (((z + zs - zr) % zs) * 2 + y, tp),
        )

    def to_a(zr):
        return remote(view(zr, 0, 0), a_send.at[zr], slot_recv.at[slot(zr, 1, 0)], a_peer)

    def to_b(zr, ar):
        return remote(
            view(zr, ar, 0), b_send.at[zr * 2 + ar], slot_recv.at[slot(zr, ar, 1)], b_peer
        )

    def to_partner(zr, ar, br):
        s = slot(zr, ar, br)
        return remote(view(zr, ar, br), d_send.at[s], d_recv.at[s], partner)

    def arrived(zr, ar, br):
        remote(
            view(zr, ar, br), z_send.at[0], slot_recv.at[slot(zr, ar, br)], partner
        ).wait_recv()

    for zr in range(1, zs):
        to_z(zr).start()
    to_a(0).start()
    to_b(0, 0).start()
    for copy in weight_copies:
        copy.start()
    to_partner(0, 0, 0).start()
    state_copy.start()
    for copy in out_copies:
        copy.start()
    acc[...] = jnp.zeros_like(acc)
    ss[...] = jnp.zeros_like(ss)
    ones = jnp.ones((2 * width, ss.shape[1]), BF16)
    for copy in weight_copies:
        copy.wait()

    @pl.loop(0, zs)
    def _(zr):
        @pl.when(zr > 0)
        def _():
            arrived(zr, 0, 0)
            to_a(zr).start()
            to_b(zr, 0).start()
            to_partner(zr, 0, 0).start()

        arrived(zr, 1, 0)
        to_b(zr, 1).start()
        to_partner(zr, 1, 0).start()
        arrived(zr, 0, 1)
        to_partner(zr, 0, 1).start()
        arrived(zr, 1, 1)
        to_partner(zr, 1, 1).start()

        @pl.loop(0, 4)
        def _(f):
            fy, fx = f // 2, f % 2
            other = columns(zr, fy, fx, 1 - c)
            remote(gath.at[:, other], z_send.at[0], d_recv.at[zr * 4 + f], partner).wait_recv()
            oz = (z + zr) % zs
            index = (oz * 2 + y + fy * (1 - 2 * y)) * (tp_size // 2) + x + fx * (1 - 2 * x)
            pair = pl.ds(pl.multiple_of(index * 2 * width, 2 * width), 2 * width)
            raw = gath[:, pair].astype(F32)
            ss[...] += jnp.dot((raw * raw).astype(BF16), ones, preferred_element_type=F32)
            lhs = (raw * gain_ref[:, pair]).astype(BF16)
            acc[:, 0:hk] += jnp.dot(lhs, wq[pair, :], preferred_element_type=F32)
            acc[:, hk : 2 * hk] += jnp.dot(lhs, wf[pair, :], preferred_element_type=F32)
            acc[:, 2 * hk :] += contract(lhs, wig[:, pair], 1, 1)

    for t in range(prop):
        r = slice(t * seqs, (t + 1) * seqs)
        scale = lax.rsqrt(ss[r, :] * (1.0 / features) + NORM_EPSILON)
        for j in range(acc.shape[1] // 128):
            cs = slice(j * 128, (j + 1) * 128)
            value = (acc[r, cs] * scale).astype(BF16).astype(F32)
            if hk <= j * 128 < 2 * hk:
                fs = slice(j * 128 - hk, j * 128 - hk + 128)
                floor = floor_ref[:, fs]
                value = floor + (1.0 - floor) * jax.nn.sigmoid(value)
            acc[r, cs] = value

    def part(t, first, size):
        return acc[t * seqs : (t + 1) * seqs, first : first + size]

    run = None
    for t in range(prop):
        gate = part(t, hk, hk)
        run = gate if run is None else run * gate
        qd[t] = part(t, 0, hk) * run
    for t in range(prop):
        total = None
        back = None
        for u in range(t, -1, -1):
            near = 1.0 - part(u, hk, hk)
            reach = part(t, 0, hk) if back is None else part(t, 0, hk) * back
            score = jnp.dot((reach * near).astype(BF16), fold_ref[...], preferred_element_type=F32)
            piece = score * part(u, 2 * hk, hv)
            total = piece if total is None else total + piece
            gate = part(u, hk, hk)
            back = gate if back is None else back * gate
        ho[t] = total

    state_copy.wait()
    wide = 8 * vals
    mask = (lax.broadcasted_iota(jnp.int32, (8 * prop, wide), 0) % 8) == (
        lax.broadcasted_iota(jnp.int32, (8 * prop, wide), 1) // vals
    )
    lane_head = lax.broadcasted_iota(jnp.int32, (8 * prop, hv), 1) // vals

    @pl.loop(0, seqs // 8)
    def _(g):
        group = pl.ds(pl.multiple_of(g * 8, 8), 8)
        result = jnp.zeros((8 * prop, hv), F32)
        for h in range(heads):
            lhs = qd[:, group, h * keys : (h + 1) * keys].reshape(8 * prop, keys).astype(BF16)
            rhs = st[group, h].reshape(wide, keys)
            o = jnp.where(mask, contract(lhs, rhs, 1, 1), 0.0)
            folded = o[:, :hv]
            for k in range(1, wide // hv):
                folded = folded + o[:, k * hv : (k + 1) * hv]
            step = hv // 2
            while step >= vals:
                folded = folded + pltpu.roll(folded, step, 1)
                step //= 2
            result = jnp.where(lane_head == h, folded, result)
        ho[:, group, :] += result.reshape(prop, 8, hv)

    pick = (
        lax.broadcasted_iota(jnp.int32, (8, hv), 0)
        == lax.broadcasted_iota(jnp.int32, (8, hv), 1) // vals
    ).astype(BF16)
    for t in range(prop):
        raw = ho[t]
        gate = part(t, 2 * hk + hv, hv)
        pre[t] = (raw * hgain_ref[...] * (gate * jax.nn.sigmoid(gate))).astype(BF16)
        sq[t] = contract(pick, (raw * raw).astype(BF16), 1, 1)

    exchanges = []
    for d in range(1, tp_size):
        to = (tp + d) % tp_size
        for src, dst, send, recv in ((pre, rx, x_send, x_recv), (sq, rsq, s_send, s_recv)):
            copy = pltpu.make_async_remote_copy(
                src_ref=src.at[to],
                dst_ref=dst.at[tp],
                send_sem=send.at[d],
                recv_sem=recv.at[d],
                device_id=(kv, to),
                device_id_type=MESH,
            )
            copy.start()
            exchanges.append(copy)
    rx[tp] = pre[tp]
    rsq[tp] = sq[tp]
    for copy in out_copies:
        copy.wait()
    for copy in exchanges:
        copy.wait()

    squares = rsq[0]
    for j in range(1, tp_size):
        squares = squares + rsq[j]
    factor = lax.rsqrt(squares * (1.0 / keys) + NORM_EPSILON)
    place = (
        lax.broadcasted_iota(jnp.int32, (8, tp_size * hv), 0)
        == (lax.broadcasted_iota(jnp.int32, (8, tp_size * hv), 1) // vals) % heads
    ).astype(BF16)
    high = factor.astype(BF16)
    low = (factor - high.astype(F32)).astype(BF16)
    factors = contract(high, place, 0, 0) + contract(low, place, 0, 0)
    flat = jnp.concatenate([rx[j] for j in range(tp_size)], axis=1).astype(F32)
    flat = (flat * factors).astype(BF16)

    home = me // 2

    def to_owner(k, core):
        chip = (home + k) % chips
        dest = chip * 2 + core
        return pltpu.make_async_remote_copy(
            src_ref=term.at[dest],
            dst_ref=rt.at[tp * kv_size + kv],
            send_sem=t_send.at[k * 2 + core],
            recv_sem=t_recv.at[k * 2 + c],
            device_id=(dest // tp_size, dest % tp_size),
            device_id_type=MESH,
        )

    @pl.loop(0, chips)
    def _(i):
        k = (i + 1) % chips
        chip = (home + k) % chips
        cols = pl.ds(pl.multiple_of(chip * 2 * width, 2 * width), 2 * width)
        pair = jnp.dot(flat, wo[:, cols], preferred_element_type=F32).astype(BF16)
        term[chip * 2] = pair[:, :width]
        term[chip * 2 + 1] = pair[:, width:]

        @pl.when(k > 0)
        def _():
            to_owner(k, 0).start()
            to_owner(k, 1).start()

    to_owner(0, 1 - c).start()
    rt[tp * kv_size + kv] = term[me]

    for zr in range(1, zs):
        to_z(zr).wait_send()
    for zr in range(zs):
        to_a(zr).wait_send()
        for ar in range(2):
            to_b(zr, ar).wait_send()
            for br in range(2):
                to_partner(zr, ar, br).wait_send()

    def landed(k, core):
        source = ((home + chips - k) % chips) * 2 + core
        block = rt.at[(source % tp_size) * kv_size + source // tp_size]
        pltpu.make_async_remote_copy(
            src_ref=block,
            dst_ref=block,
            send_sem=t_send.at[k * 2 + core],
            recv_sem=t_recv.at[k * 2 + core],
            device_id=partner,
            device_id_type=MESH,
        ).wait_recv()

    landed(0, 1 - c)
    to_owner(0, 1 - c).wait_send()

    @pl.loop(1, chips)
    def _(k):
        landed(k, 0)
        landed(k, 1)
        to_owner(k, 0).wait_send()
        to_owner(k, 1).wait_send()

    for j in range(tp_size):
        total = rt[j * kv_size].astype(F32)
        for i in range(1, kv_size):
            total = total + rt[j * kv_size + i].astype(F32)
        out_ref[j * seqs : (j + 1) * seqs, :] = total.astype(BF16)


def fused(
    kv_size,
    tp_size,
    tokens,
    input_norm_gain,
    w_query,
    w_forget,
    w_input,
    w_gate,
    forget_floor,
    head_gain,
    w_out,
    state,
    prev_forget,
    prev_input,
    accepted,
):
    seqs, prop, width = tokens.shape
    heads, vals, keys = state.shape[1:]
    n = kv_size * tp_size
    rows, features = seqs * prop, n * width
    hk, hv = heads * keys, heads * vals
    new_state, low_state = update_state(accepted, prev_forget, prev_input, state)
    fold = (jnp.arange(hk)[:, None] // keys == jnp.arange(hv)[None, :] // vals).astype(BF16)
    vmem = pl.BlockSpec(memory_space=pltpu.VMEM)
    hbm = pl.BlockSpec(memory_space=pl.ANY)
    dma = pltpu.SemaphoreType.DMA
    slots = kv_size * tp_size // 2
    out = pl.pallas_call(
        functools.partial(layer_kernel, kv_size, tp_size),
        out_shape=jax.ShapeDtypeStruct((rows, width), BF16),
        in_specs=[vmem] * 5 + [hbm] * 6,
        out_specs=vmem,
        scratch_shapes=[
            pltpu.VMEM((rows, features), BF16),
            pltpu.VMEM((features, hk), BF16),
            pltpu.VMEM((features, hk), BF16),
            pltpu.VMEM((2 * hv, features), BF16),
            pltpu.VMEM((hk, features), BF16),
            pltpu.VMEM((seqs, heads, vals, keys), BF16),
            pltpu.VMEM((rows, 2 * hk + 2 * hv), F32),
            pltpu.VMEM((rows, 128), F32),
            pltpu.VMEM((prop, seqs, hk), F32),
            pltpu.VMEM((prop, seqs, hv), F32),
            pltpu.VMEM((prop, seqs, hv), BF16),
            pltpu.VMEM((prop, 8, seqs), F32),
            pltpu.VMEM((tp_size, seqs, hv), BF16),
            pltpu.VMEM((tp_size, 8, seqs), F32),
            pltpu.VMEM((n, seqs, width), BF16),
            pltpu.VMEM((n, seqs, width), BF16),
            dma((5,)),
            dma((heads * tp_size,)),
            dma,
            dma((kv_size // 2,)),
            dma((kv_size // 2,)),
            dma((kv_size,)),
            dma((slots,)),
            dma((slots,)),
            dma((slots,)),
            dma((tp_size,)),
            dma((tp_size,)),
            dma((tp_size,)),
            dma((tp_size,)),
            dma((n,)),
            dma((n,)),
        ],
        compiler_params=pltpu.CompilerParams(
            collective_id=0, has_side_effects=True, vmem_limit_bytes=VMEM_BYTES
        ),
        cost_estimate=pl.CostEstimate(
            flops=2 * rows * features * (2 * hk + 3 * hv),
            bytes_accessed=2 * features * (3 * hk + 2 * hv),
            transcendentals=0,
        ),
    )(
        tokens.transpose(1, 0, 2).reshape(rows, width),
        input_norm_gain.reshape(1, features),
        forget_floor.reshape(1, hk),
        jnp.tile(head_gain, heads).reshape(1, hv),
        fold,
        w_query,
        w_forget,
        w_input.reshape(hv, features),
        w_gate.reshape(hv, features),
        w_out,
        low_state,
    )
    return out.reshape(prop, seqs, width).transpose(1, 0, 2), new_state


def fits(kv_size, tp_size, tokens, state):
    seqs, prop, width = tokens.shape
    heads, vals, keys = state.shape[1:]
    return (
        kv_size % 2 == 0
        and tp_size == 4
        and prop == tp_size
        and width == 128
        and seqs == 128
        and keys == 128
        and heads * vals == 128
        and vals % 32 == 0
        and heads <= 8
    )


def rms_scale(values, gain):
    return (
        values * lax.rsqrt(jnp.mean(values * values, axis=-1, keepdims=True) + NORM_EPSILON) * gain
    )


def by_rows(normed, weight):
    return lax.dot_general(
        normed, weight, (((1,), (1,)), ((), ())), preferred_element_type=jnp.float32
    )


def general(
    tokens,
    input_norm_gain,
    w_query,
    w_forget,
    w_input,
    w_gate,
    forget_floor,
    head_gain,
    w_out,
    state,
    prev_forget,
    prev_input,
    accepted,
):
    seq_count = tokens.shape[0]
    proposals = tokens.shape[1]
    whole = lax.all_gather(tokens, ("kv", "tp"), axis=2, tiled=True)
    widths = whole.shape[2]
    row_count = seq_count * proposals
    normed = (
        rms_scale(whole.astype(jnp.float32), input_norm_gain)
        .astype(jnp.bfloat16)
        .reshape(row_count, widths)
    )
    heads_local = state.shape[1]
    value_local = state.shape[2]
    head_size = state.shape[3]
    group_members = lax.axis_size("tp")
    queries = jnp.dot(normed, w_query, preferred_element_type=jnp.float32).astype(jnp.bfloat16)
    forget_raw = jnp.dot(normed, w_forget, preferred_element_type=jnp.float32).astype(jnp.bfloat16)
    input_proj = by_rows(normed, w_input.reshape(heads_local * value_local, widths)).astype(
        jnp.bfloat16
    )
    gate_raw = by_rows(normed, w_gate.reshape(heads_local * value_local, widths)).astype(
        jnp.bfloat16
    )
    head_shape = (seq_count, proposals, heads_local, head_size)
    value_shape = (seq_count, proposals, heads_local, value_local)
    forget = forget_floor + (1.0 - forget_floor) * jax.nn.sigmoid(forget_raw.astype(jnp.float32))
    forget = forget.reshape(head_shape)
    log_forget = jnp.log(forget)
    keys_now = 1.0 - forget
    values_now = input_proj.astype(jnp.float32).reshape(value_shape)
    query_vector = queries.astype(jnp.float32).reshape(head_shape)
    previous = prev_forget.reshape(head_shape)
    prev_values = prev_input.astype(jnp.float32)
    alive_mask = (jnp.arange(proposals)[None, :] < accepted[:, None])[:, :, None, None]
    prev_log = jnp.where(alive_mask, jnp.log(previous), 0.0)
    prev_cum = jnp.cumsum(prev_log, axis=1)
    prev_total = prev_cum[:, -1]
    weights_prev = jnp.where(
        alive_mask, jnp.exp(prev_total[:, None] - prev_cum) * (1.0 - previous), 0.0
    )
    new_state = jnp.exp(prev_total)[:, :, None, :] * state + jnp.einsum(
        "sphk,sphv->shvk", weights_prev, prev_values
    )
    decay_cum = jnp.cumsum(log_forget, axis=1)
    carried = jnp.einsum("sthk,shvk->sthv", query_vector * jnp.exp(decay_cum), new_state)
    triangle = jnp.tril(jnp.ones((proposals, proposals), dtype=bool))[None, :, :, None, None]
    spread = jnp.where(triangle, decay_cum[:, :, None] - decay_cum[:, None, :], 0.0)
    relative = jnp.where(triangle, jnp.exp(spread), 0.0)
    scores = jnp.einsum("sthk,suhk,stuhk->stuh", query_vector, keys_now, relative)
    heads_out = carried + jnp.einsum("stuh,suhv->sthv", scores, values_now)
    square_sum = lax.psum(jnp.sum(heads_out * heads_out, axis=-1), "tp")
    norm_factor = lax.rsqrt(square_sum / head_size + NORM_EPSILON)
    gate_heads = gate_raw.astype(jnp.float32).reshape(value_shape)
    hidden = (heads_out * norm_factor[..., None] * head_gain * jax.nn.silu(gate_heads)).astype(
        jnp.bfloat16
    )
    hidden_heads = hidden.reshape(row_count, heads_local, value_local)
    regrouped = lax.all_to_all(hidden_heads, "tp", split_axis=0, concat_axis=2, tiled=True)
    flat = regrouped.reshape(row_count // group_members, heads_local * head_size)
    term = jnp.dot(flat, w_out, preferred_element_type=jnp.float32)
    summed = lax.psum_scatter(term.astype(jnp.bfloat16), "kv", scatter_dimension=1, tiled=True)
    placed = lax.all_to_all(summed, "tp", split_axis=1, concat_axis=0, tiled=True)
    mixed = placed.reshape(seq_count, proposals, -1)
    return (mixed, new_state)


def solution(mesh):
    placed = (
        P(None, None, ("kv", "tp")),
        P(),
        P(None, "kv"),
        P(None, "kv"),
        P("kv", "tp", None),
        P("kv", "tp", None),
        P("kv"),
        P("tp"),
        P("kv", None),
        P(None, "kv", "tp", None),
        P(None, None, "kv"),
        P(None, None, "kv", "tp"),
        P(),
    )
    kv_size, tp_size = mesh.shape["kv"], mesh.shape["tp"]

    def body(*args):
        if fits(kv_size, tp_size, args[0], args[9]):
            return fused(kv_size, tp_size, *args)
        return general(*args)

    return jax.shard_map(
        body,
        mesh=mesh,
        in_specs=placed,
        out_specs=(P(None, None, ("kv", "tp")), P(None, "kv", "tp", None)),
        check_vma=False,
    )
```

```python
import functools

import jax
import jax.numpy as jnp
from jax import lax
from jax.experimental import pallas as pl
from jax.experimental.pallas import tpu as pltpu
from jax.sharding import PartitionSpec as P

NORM_EPSILON = 1e-06
MESH = pl.DeviceIdType.MESH
VMEM_BYTES = 60 * 1024 * 1024
F32 = jnp.float32
BF16 = jnp.bfloat16


def contract(a, b, da, db):
    return lax.dot_general(a, b, (((da,), (db,)), ((), ())), preferred_element_type=F32)


def state_kernel(acc_ref, pf_ref, pv_ref, spread_ref, state_ref, new_ref, low_ref):
    prop, group, chans = pf_ref.shape
    heads, vals, keys = state_ref.shape[1:]
    wide = 8 * vals
    accepted = acc_ref[...]
    decay = jnp.ones((group, chans), F32)
    weights = [None] * prop
    for p in range(prop - 1, -1, -1):
        alive = p < accepted
        gate = pf_ref[p]
        weights[p] = jnp.where(alive, decay * (1.0 - gate), 0.0)
        decay = jnp.where(alive, decay * gate, decay)
    spread = [
        jnp.dot(pv_ref[p], spread_ref[...], preferred_element_type=F32) for p in range(prop)
    ]
    rows = lax.broadcasted_iota(jnp.int32, (8 * prop, wide), 0) % 8
    lanes = lax.broadcasted_iota(jnp.int32, (8 * prop, wide), 1) // vals
    mask = rows == lanes
    for g in range(group // 8):
        sl = slice(g * 8, g * 8 + 8)
        for h in range(heads):
            hk = slice(h * keys, (h + 1) * keys)
            lhs = jnp.concatenate(
                [spread[p][sl, h * wide : (h + 1) * wide] for p in range(prop)], axis=0
            )
            lhs = jnp.where(mask, lhs, 0.0).astype(BF16)
            rhs = jnp.concatenate([weights[p][sl, hk] for p in range(prop)], axis=0).astype(BF16)
            update = contract(lhs, rhs, 0, 0).reshape(8, vals, keys)
            new = decay[sl, hk][:, None, :] * state_ref[sl, h] + update
            new_ref[sl, h] = new
            low_ref[sl, h] = new.astype(BF16)


def update_state(accepted, prev_forget, prev_input, state):
    seqs, heads, vals, keys = state.shape
    prop = prev_forget.shape[1]
    group = 16
    pf = prev_forget.transpose(1, 0, 2)
    pv = prev_input.reshape(seqs, prop, heads * vals).transpose(1, 0, 2)
    r = jnp.arange(heads * vals)[:, None]
    c = jnp.arange(heads * 8 * vals)[None, :]
    spread = ((r // vals == c // (8 * vals)) & (r % vals == c % vals)).astype(BF16)
    block = (group, heads, vals, keys)
    return pl.pallas_call(
        state_kernel,
        grid=(seqs // group,),
        in_specs=[
            pl.BlockSpec((group, 1), lambda i: (i, 0)),
            pl.BlockSpec((prop, group, heads * keys), lambda i: (0, i, 0)),
            pl.BlockSpec((prop, group, heads * vals), lambda i: (0, i, 0)),
            pl.BlockSpec(spread.shape, lambda i: (0, 0)),
            pl.BlockSpec(block, lambda i: (i, 0, 0, 0)),
        ],
        out_specs=[
            pl.BlockSpec(block, lambda i: (i, 0, 0, 0)),
            pl.BlockSpec(block, lambda i: (i, 0, 0, 0)),
        ],
        out_shape=[
            jax.ShapeDtypeStruct(state.shape, F32),
            jax.ShapeDtypeStruct(state.shape, BF16),
        ],
        compiler_params=pltpu.CompilerParams(vmem_limit_bytes=VMEM_BYTES),
        cost_estimate=pl.CostEstimate(
            flops=2 * 8 * prop * state.size, bytes_accessed=10 * state.size, transcendentals=0
        ),
    )(accepted.reshape(seqs, 1), pf, pv, spread, state)


def layer_kernel(
    kv_size,
    tp_size,
    tok_ref,
    gain_ref,
    floor_ref,
    hgain_ref,
    wq_hbm,
    wf_hbm,
    wi_hbm,
    wg_hbm,
    wo_hbm,
    st_hbm,
    out_ref,
    gath,
    wq,
    wf,
    wig,
    wo,
    st,
    acc,
    ss,
    qd,
    ho,
    pre,
    sq,
    rx,
    rsq,
    term,
    mine,
    half,
    quarter,
    done,
    rt,
    w_sem,
    wo_sem,
    own_sem,
    z_send,
    a_send,
    b_send,
    d_send,
    slot_recv,
    d_recv,
    x_send,
    x_recv,
    s_send,
    s_recv,
    t_send,
    t_recv,
):
    n = kv_size * tp_size
    zs = kv_size // 2
    kv = lax.axis_index("kv")
    tp = lax.axis_index("tp")
    me = kv * tp_size + tp
    z, y, x, c = kv // 2, kv % 2, tp // 2, tp % 2
    width = tok_ref.shape[1]
    rows = tok_ref.shape[0]
    seqs, heads, vals, keys = st_hbm.shape
    prop = rows // seqs
    hk = heads * keys
    hv = heads * vals
    features = n * width

    weight_copies = [
        pltpu.make_async_copy(wq_hbm, wq, w_sem.at[0]),
        pltpu.make_async_copy(wf_hbm, wf, w_sem.at[1]),
        pltpu.make_async_copy(wi_hbm, wig.at[pl.ds(0, hv)], w_sem.at[2]),
        pltpu.make_async_copy(wg_hbm, wig.at[pl.ds(hv, hv)], w_sem.at[3]),
    ]
    state_copy = pltpu.make_async_copy(st_hbm, st, w_sem.at[4])
    out_copies = [
        pltpu.make_async_copy(
            wo_hbm.at[pl.ds(h * keys + j * vals, vals)],
            wo.at[pl.ds((j * heads + h) * vals, vals)],
            wo_sem.at[h * tp_size + j],
        )
        for h in range(heads)
        for j in range(tp_size)
    ]

    def columns(zr, fy, fx, core):
        oz = (z + zr) % zs
        oy = y + fy * (1 - 2 * y)
        ox = x + fx * (1 - 2 * x)
        index = (oz * 2 + oy) * tp_size + ox * 2 + core
        return pl.ds(pl.multiple_of(index * width, width), width)

    own = pltpu.make_async_copy(tok_ref, gath.at[:, columns(0, 0, 0, c)], own_sem)
    own.start()

    barrier = pltpu.get_barrier_semaphore()

    @pl.loop(1, n)
    def _(d):
        other = (me + d) % n
        pl.semaphore_signal(
            barrier,
            inc=1,
            device_id=(other // tp_size, other % tp_size),
            device_id_type=MESH,
        )

    own.wait()
    pl.semaphore_wait(barrier, n - 1)

    def remote(view, send, recv, target):
        return pltpu.make_async_remote_copy(
            src_ref=view,
            dst_ref=view,
            send_sem=send,
            recv_sem=recv,
            device_id=target,
            device_id_type=MESH,
        )

    a_peer = (kv + (1 - c) * (1 - 2 * y), tp + c * (1 - 2 * x) * 2)
    b_peer = (kv + c * (1 - 2 * y), tp + (1 - c) * (1 - 2 * x) * 2)
    partner = (kv, tp + 1 - 2 * c)

    def flips(ar, br):
        return ar * (1 - c) + br * c, ar * c + br * (1 - c)

    def view(zr, ar, br):
        fy, fx = flips(ar, br)
        return gath.at[:, columns(zr, fy, fx, c)]

    def slot(zr, ar, br):
        fy, fx = flips(ar, br)
        return zr * 4 + fy * 2 + fx

    def to_z(zr):
        return remote(
            view(0, 0, 0),
            z_send.at[zr],
            slot_recv.at[zr * 4],
            (((z + zs - zr) % zs) * 2 + y, tp),
        )

    def to_a(zr):
        return remote(view(zr, 0, 0), a_send.at[zr], slot_recv.at[slot(zr, 1, 0)], a_peer)

    def to_b(zr, ar):
        return remote(
            view(zr, ar, 0), b_send.at[zr * 2 + ar], slot_recv.at[slot(zr, ar, 1)], b_peer
        )

    def to_partner(zr, ar, br):
        s = slot(zr, ar, br)
        return remote(view(zr, ar, br), d_send.at[s], d_recv.at[s], partner)

    def arrived(zr, ar, br):
        remote(
            view(zr, ar, br), z_send.at[0], slot_recv.at[slot(zr, ar, br)], partner
        ).wait_recv()

    for zr in range(1, zs):
        to_z(zr).start()
    to_a(0).start()
    to_b(0, 0).start()
    for copy in weight_copies:
        copy.start()
    to_partner(0, 0, 0).start()
    state_copy.start()
    for copy in out_copies:
        copy.start()
    acc[...] = jnp.zeros_like(acc)
    ss[...] = jnp.zeros_like(ss)
    ones = jnp.ones((2 * width, ss.shape[1]), BF16)
    for copy in weight_copies:
        copy.wait()

    @pl.loop(0, zs)
    def _(zr):
        @pl.when(zr > 0)
        def _():
            arrived(zr, 0, 0)
            to_a(zr).start()
            to_b(zr, 0).start()
            to_partner(zr, 0, 0).start()

        arrived(zr, 1, 0)
        to_b(zr, 1).start()
        to_partner(zr, 1, 0).start()
        arrived(zr, 0, 1)
        to_partner(zr, 0, 1).start()
        arrived(zr, 1, 1)
        to_partner(zr, 1, 1).start()

        @pl.loop(0, 4)
        def _(f):
            fy, fx = f // 2, f % 2
            other = columns(zr, fy, fx, 1 - c)
            remote(gath.at[:, other], z_send.at[0], d_recv.at[zr * 4 + f], partner).wait_recv()
            oz = (z + zr) % zs
            index = (oz * 2 + y + fy * (1 - 2 * y)) * (tp_size // 2) + x + fx * (1 - 2 * x)
            pair = pl.ds(pl.multiple_of(index * 2 * width, 2 * width), 2 * width)
            raw = gath[:, pair].astype(F32)
            ss[...] += jnp.dot((raw * raw).astype(BF16), ones, preferred_element_type=F32)
            lhs = (raw * gain_ref[:, pair]).astype(BF16)
            acc[:, 0:hk] += jnp.dot(lhs, wq[pair, :], preferred_element_type=F32)
            acc[:, hk : 2 * hk] += jnp.dot(lhs, wf[pair, :], preferred_element_type=F32)
            acc[:, 2 * hk :] += contract(lhs, wig[:, pair], 1, 1)

    for t in range(prop):
        r = slice(t * seqs, (t + 1) * seqs)
        scale = lax.rsqrt(ss[r, :] * (1.0 / features) + NORM_EPSILON)
        for j in range(acc.shape[1] // 128):
            cs = slice(j * 128, (j + 1) * 128)
            value = (acc[r, cs] * scale).astype(BF16).astype(F32)
            if hk <= j * 128 < 2 * hk:
                fs = slice(j * 128 - hk, j * 128 - hk + 128)
                floor = floor_ref[:, fs]
                value = floor + (1.0 - floor) * jax.nn.sigmoid(value)
            acc[r, cs] = value

    def part(t, first, size):
        return acc[t * seqs : (t + 1) * seqs, first : first + size]

    run = None
    for t in range(prop):
        gate = part(t, hk, hk)
        run = gate if run is None else run * gate
        qd[t] = part(t, 0, hk) * run
    fold = (
        lax.broadcasted_iota(jnp.int32, (hk, hv), 0) // keys
        == lax.broadcasted_iota(jnp.int32, (hk, hv), 1) // vals
    ).astype(BF16)
    for t in range(prop):
        total = None
        back = None
        for u in range(t, -1, -1):
            near = 1.0 - part(u, hk, hk)
            reach = part(t, 0, hk) if back is None else part(t, 0, hk) * back
            score = jnp.dot((reach * near).astype(BF16), fold, preferred_element_type=F32)
            piece = score * part(u, 2 * hk, hv)
            total = piece if total is None else total + piece
            gate = part(u, hk, hk)
            back = gate if back is None else back * gate
        ho[t] = total

    state_copy.wait()
    wide = 8 * vals
    mask = (lax.broadcasted_iota(jnp.int32, (8 * prop, wide), 0) % 8) == (
        lax.broadcasted_iota(jnp.int32, (8 * prop, wide), 1) // vals
    )
    lane_head = lax.broadcasted_iota(jnp.int32, (8 * prop, hv), 1) // vals

    @pl.loop(0, seqs // 8, unroll=2)
    def _(g):
        group = pl.ds(pl.multiple_of(g * 8, 8), 8)
        result = jnp.zeros((8 * prop, hv), F32)
        for h in range(heads):
            lhs = qd[:, group, h * keys : (h + 1) * keys].reshape(8 * prop, keys).astype(BF16)
            rhs = st[group, h].reshape(wide, keys)
            o = jnp.where(mask, contract(lhs, rhs, 1, 1), 0.0)
            folded = o[:, :hv]
            for k in range(1, wide // hv):
                folded = folded + o[:, k * hv : (k + 1) * hv]
            step = hv // 2
            while step >= vals:
                folded = folded + pltpu.roll(folded, step, 1)
                step //= 2
            result = jnp.where(lane_head == h, folded, result)
        ho[:, group, :] += result.reshape(prop, 8, hv)

    pick = (
        lax.broadcasted_iota(jnp.int32, (8, hv), 0)
        == lax.broadcasted_iota(jnp.int32, (8, hv), 1) // vals
    ).astype(BF16)
    head_gain = jnp.concatenate([hgain_ref[...]] * heads, axis=1)
    for t in range(prop):
        raw = ho[t]
        gate = part(t, 2 * hk + hv, hv)
        pre[t] = (raw * head_gain * (gate * jax.nn.sigmoid(gate))).astype(BF16)
        sq[t] = contract(pick, (raw * raw).astype(BF16), 1, 1)

    exchanges = []
    for d in range(1, tp_size):
        to = (tp + d) % tp_size
        for src, dst, send, recv in ((pre, rx, x_send, x_recv), (sq, rsq, s_send, s_recv)):
            copy = pltpu.make_async_remote_copy(
                src_ref=src.at[to],
                dst_ref=dst.at[tp],
                send_sem=send.at[d],
                recv_sem=recv.at[d],
                device_id=(kv, to),
                device_id_type=MESH,
            )
            copy.start()
            exchanges.append(copy)
    rx[tp] = pre[tp]
    rsq[tp] = sq[tp]
    for copy in out_copies:
        copy.wait()
    for copy in exchanges:
        copy.wait()

    squares = rsq[0]
    for j in range(1, tp_size):
        squares = squares + rsq[j]
    factor = lax.rsqrt(squares * (1.0 / keys) + NORM_EPSILON)
    place = (
        lax.broadcasted_iota(jnp.int32, (8, tp_size * hv), 0)
        == (lax.broadcasted_iota(jnp.int32, (8, tp_size * hv), 1) // vals) % heads
    ).astype(BF16)
    high = factor.astype(BF16)
    low = (factor - high.astype(F32)).astype(BF16)
    factors = contract(high, place, 0, 0) + contract(low, place, 0, 0)
    flat = jnp.concatenate([rx[j] for j in range(tp_size)], axis=1).astype(F32)
    flat = (flat * factors).astype(BF16)

    y_peer = (kv + 1 - 2 * y, tp)
    order = list(range(1, zs)) + [0]

    def blocks(dz, side):
        start = (((z + dz) % zs) * 2 + side) * tp_size
        return pl.ds(start, tp_size)

    def to_y(dz):
        return pltpu.make_async_remote_copy(
            src_ref=term.at[blocks(dz, 1 - y)],
            dst_ref=half.at[dz],
            send_sem=t_send.at[dz],
            recv_sem=t_recv.at[dz],
            device_id=y_peer,
            device_id_type=MESH,
        )

    def along_z(dz):
        return pltpu.make_async_remote_copy(
            src_ref=term.at[blocks(dz, y)],
            dst_ref=quarter.at[dz],
            send_sem=t_send.at[zs + dz],
            recv_sem=t_recv.at[zs + dz],
            device_id=(((z + dz) % zs) * 2 + y, tp),
            device_id_type=MESH,
        )

    def product(dz, side):
        first = (((z + dz) % zs) * 2 + side) * tp_size * width
        cols = pl.ds(pl.multiple_of(first, tp_size * width), tp_size * width)
        return jnp.dot(flat, wo[:, cols], preferred_element_type=F32)

    for dz in order:
        away = product(dz, 1 - y).astype(BF16)
        base = (((z + dz) % zs) * 2 + 1 - y) * tp_size
        for j in range(tp_size):
            term[base + j] = away[:, j * width : (j + 1) * width]
        to_y(dz).start()
    for dz in order:
        mine[dz] = product(dz, y)
    for dz in order:
        to_y(dz).wait_recv()
        base = (((z + dz) % zs) * 2 + y) * tp_size
        for j in range(tp_size):
            cs = slice(j * width, (j + 1) * width)
            total = mine[dz, :, cs] + half[dz, j].astype(F32)
            if dz > 0:
                term[base + j] = total.astype(BF16)
            else:
                mine[dz, :, cs] = total
        if dz > 0:
            along_z(dz).start()
    for dz in range(1, zs):
        along_z(dz).wait_recv()
    for j in range(tp_size):
        total = mine[0, :, j * width : (j + 1) * width]
        for dz in range(1, zs):
            total = total + quarter[dz, j].astype(F32)
        done[j] = total.astype(BF16)

    finals = []
    for d in range(1, tp_size):
        to = (tp + d) % tp_size
        copy = pltpu.make_async_remote_copy(
            src_ref=done.at[to],
            dst_ref=rt.at[tp],
            send_sem=t_send.at[2 * zs + d],
            recv_sem=t_recv.at[2 * zs + d],
            device_id=(kv, to),
            device_id_type=MESH,
        )
        copy.start()
        finals.append(copy)
    rt[tp] = done[tp]

    for zr in range(1, zs):
        to_z(zr).wait_send()
    for zr in range(zs):
        to_a(zr).wait_send()
        for ar in range(2):
            to_b(zr, ar).wait_send()
            for br in range(2):
                to_partner(zr, ar, br).wait_send()

    for dz in range(zs):
        to_y(dz).wait_send()
        if dz > 0:
            along_z(dz).wait_send()
    for copy in finals:
        copy.wait()
    for j in range(tp_size):
        out_ref[j * seqs : (j + 1) * seqs, :] = rt[j]


def fused(
    kv_size,
    tp_size,
    tokens,
    input_norm_gain,
    w_query,
    w_forget,
    w_input,
    w_gate,
    forget_floor,
    head_gain,
    w_out,
    state,
    prev_forget,
    prev_input,
    accepted,
):
    seqs, prop, width = tokens.shape
    heads, vals, keys = state.shape[1:]
    n = kv_size * tp_size
    rows, features = seqs * prop, n * width
    hk, hv = heads * keys, heads * vals
    new_state, low_state = update_state(accepted, prev_forget, prev_input, state)
    vmem = pl.BlockSpec(memory_space=pltpu.VMEM)
    hbm = pl.BlockSpec(memory_space=pl.ANY)
    dma = pltpu.SemaphoreType.DMA
    slots = kv_size * tp_size // 2
    out = pl.pallas_call(
        functools.partial(layer_kernel, kv_size, tp_size),
        out_shape=jax.ShapeDtypeStruct((rows, width), BF16),
        in_specs=[vmem] * 4 + [hbm] * 6,
        out_specs=vmem,
        scratch_shapes=[
            pltpu.VMEM((rows, features), BF16),
            pltpu.VMEM((features, hk), BF16),
            pltpu.VMEM((features, hk), BF16),
            pltpu.VMEM((2 * hv, features), BF16),
            pltpu.VMEM((hk, features), BF16),
            pltpu.VMEM((seqs, heads, vals, keys), BF16),
            pltpu.VMEM((rows, 2 * hk + 2 * hv), F32),
            pltpu.VMEM((rows, 128), F32),
            pltpu.VMEM((prop, seqs, hk), F32),
            pltpu.VMEM((prop, seqs, hv), F32),
            pltpu.VMEM((prop, seqs, hv), BF16),
            pltpu.VMEM((prop, 8, seqs), F32),
            pltpu.VMEM((tp_size, seqs, hv), BF16),
            pltpu.VMEM((tp_size, 8, seqs), F32),
            pltpu.VMEM((n, seqs, width), BF16),
            pltpu.VMEM((kv_size // 2, seqs, tp_size * width), F32),
            pltpu.VMEM((kv_size // 2, tp_size, seqs, width), BF16),
            pltpu.VMEM((kv_size // 2, tp_size, seqs, width), BF16),
            pltpu.VMEM((tp_size, seqs, width), BF16),
            pltpu.VMEM((tp_size, seqs, width), BF16),
            dma((5,)),
            dma((heads * tp_size,)),
            dma,
            dma((kv_size // 2,)),
            dma((kv_size // 2,)),
            dma((kv_size,)),
            dma((slots,)),
            dma((slots,)),
            dma((slots,)),
            dma((tp_size,)),
            dma((tp_size,)),
            dma((tp_size,)),
            dma((tp_size,)),
            dma((kv_size + tp_size,)),
            dma((kv_size + tp_size,)),
        ],
        compiler_params=pltpu.CompilerParams(
            collective_id=0, has_side_effects=True, vmem_limit_bytes=VMEM_BYTES
        ),
        cost_estimate=pl.CostEstimate(
            flops=2 * rows * features * (2 * hk + 3 * hv),
            bytes_accessed=2 * features * (3 * hk + 2 * hv),
            transcendentals=0,
        ),
    )(
        tokens.transpose(1, 0, 2).reshape(rows, width),
        input_norm_gain.reshape(1, features),
        forget_floor.reshape(1, hk),
        head_gain.reshape(1, vals),
        w_query,
        w_forget,
        w_input.reshape(hv, features),
        w_gate.reshape(hv, features),
        w_out,
        low_state,
    )
    return out.reshape(prop, seqs, width).transpose(1, 0, 2), new_state


def fits(kv_size, tp_size, tokens, state):
    seqs, prop, width = tokens.shape
    heads, vals, keys = state.shape[1:]
    return (
        kv_size % 2 == 0
        and tp_size == 4
        and prop == tp_size
        and width == 128
        and seqs == 128
        and keys == 128
        and heads * vals == 128
        and vals % 32 == 0
        and heads <= 8
    )


def rms_scale(values, gain):
    return (
        values * lax.rsqrt(jnp.mean(values * values, axis=-1, keepdims=True) + NORM_EPSILON) * gain
    )


def by_rows(normed, weight):
    return lax.dot_general(
        normed, weight, (((1,), (1,)), ((), ())), preferred_element_type=jnp.float32
    )


def general(
    tokens,
    input_norm_gain,
    w_query,
    w_forget,
    w_input,
    w_gate,
    forget_floor,
    head_gain,
    w_out,
    state,
    prev_forget,
    prev_input,
    accepted,
):
    seq_count = tokens.shape[0]
    proposals = tokens.shape[1]
    whole = lax.all_gather(tokens, ("kv", "tp"), axis=2, tiled=True)
    widths = whole.shape[2]
    row_count = seq_count * proposals
    normed = (
        rms_scale(whole.astype(jnp.float32), input_norm_gain)
        .astype(jnp.bfloat16)
        .reshape(row_count, widths)
    )
    heads_local = state.shape[1]
    value_local = state.shape[2]
    head_size = state.shape[3]
    group_members = lax.axis_size("tp")
    queries = jnp.dot(normed, w_query, preferred_element_type=jnp.float32).astype(jnp.bfloat16)
    forget_raw = jnp.dot(normed, w_forget, preferred_element_type=jnp.float32).astype(jnp.bfloat16)
    input_proj = by_rows(normed, w_input.reshape(heads_local * value_local, widths)).astype(
        jnp.bfloat16
    )
    gate_raw = by_rows(normed, w_gate.reshape(heads_local * value_local, widths)).astype(
        jnp.bfloat16
    )
    head_shape = (seq_count, proposals, heads_local, head_size)
    value_shape = (seq_count, proposals, heads_local, value_local)
    forget = forget_floor + (1.0 - forget_floor) * jax.nn.sigmoid(forget_raw.astype(jnp.float32))
    forget = forget.reshape(head_shape)
    log_forget = jnp.log(forget)
    keys_now = 1.0 - forget
    values_now = input_proj.astype(jnp.float32).reshape(value_shape)
    query_vector = queries.astype(jnp.float32).reshape(head_shape)
    previous = prev_forget.reshape(head_shape)
    prev_values = prev_input.astype(jnp.float32)
    alive_mask = (jnp.arange(proposals)[None, :] < accepted[:, None])[:, :, None, None]
    prev_log = jnp.where(alive_mask, jnp.log(previous), 0.0)
    prev_cum = jnp.cumsum(prev_log, axis=1)
    prev_total = prev_cum[:, -1]
    weights_prev = jnp.where(
        alive_mask, jnp.exp(prev_total[:, None] - prev_cum) * (1.0 - previous), 0.0
    )
    new_state = jnp.exp(prev_total)[:, :, None, :] * state + jnp.einsum(
        "sphk,sphv->shvk", weights_prev, prev_values
    )
    decay_cum = jnp.cumsum(log_forget, axis=1)
    carried = jnp.einsum("sthk,shvk->sthv", query_vector * jnp.exp(decay_cum), new_state)
    triangle = jnp.tril(jnp.ones((proposals, proposals), dtype=bool))[None, :, :, None, None]
    spread = jnp.where(triangle, decay_cum[:, :, None] - decay_cum[:, None, :], 0.0)
    relative = jnp.where(triangle, jnp.exp(spread), 0.0)
    scores = jnp.einsum("sthk,suhk,stuhk->stuh", query_vector, keys_now, relative)
    heads_out = carried + jnp.einsum("stuh,suhv->sthv", scores, values_now)
    square_sum = lax.psum(jnp.sum(heads_out * heads_out, axis=-1), "tp")
    norm_factor = lax.rsqrt(square_sum / head_size + NORM_EPSILON)
    gate_heads = gate_raw.astype(jnp.float32).reshape(value_shape)
    hidden = (heads_out * norm_factor[..., None] * head_gain * jax.nn.silu(gate_heads)).astype(
        jnp.bfloat16
    )
    hidden_heads = hidden.reshape(row_count, heads_local, value_local)
    regrouped = lax.all_to_all(hidden_heads, "tp", split_axis=0, concat_axis=2, tiled=True)
    flat = regrouped.reshape(row_count // group_members, heads_local * head_size)
    term = jnp.dot(flat, w_out, preferred_element_type=jnp.float32)
    summed = lax.psum_scatter(term.astype(jnp.bfloat16), "kv", scatter_dimension=1, tiled=True)
    placed = lax.all_to_all(summed, "tp", split_axis=1, concat_axis=0, tiled=True)
    mixed = placed.reshape(seq_count, proposals, -1)
    return (mixed, new_state)


def solution(mesh):
    placed = (
        P(None, None, ("kv", "tp")),
        P(),
        P(None, "kv"),
        P(None, "kv"),
        P("kv", "tp", None),
        P("kv", "tp", None),
        P("kv"),
        P("tp"),
        P("kv", None),
        P(None, "kv", "tp", None),
        P(None, None, "kv"),
        P(None, None, "kv", "tp"),
        P(),
    )
    kv_size, tp_size = mesh.shape["kv"], mesh.shape["tp"]

    def body(*args):
        if fits(kv_size, tp_size, args[0], args[9]):
            return fused(kv_size, tp_size, *args)
        return general(*args)

    return jax.shard_map(
        body,
        mesh=mesh,
        in_specs=placed,
        out_specs=(P(None, None, ("kv", "tp")), P(None, "kv", "tp", None)),
        check_vma=False,
    )
```
